512 devices in a mesh: sp: 16 (over z), fs: 4 (over y), tp: 8 (over x, core).
Axes of the slice: x: 4, y: 4, z: 16, core: 2. Of those that a mesh axis runs over, the one named last changes fastest.
Arguments:
- stream: bfloat16 [4, 4096, 4096], P('fs', 'sp'), may hold values from -6 to 6
- norm_gain: float32 [4096], replicated, may hold values from 0.1 to 1.9
- value_proj: bfloat16 [4096, 1024], P(('sp', 'fs'), 'tp'), may hold values from -0.09375 to 0.09375
- gate_proj: bfloat16 [4096, 1024], P(('sp', 'fs'), 'tp'), may hold values from -0.09375 to 0.09375
- state_proj: bfloat16 [4096, 1024], P(('sp', 'fs'), 'tp'), may hold values from -0.09375 to 0.09375
- conv_kernel: bfloat16 [31, 1024], P(None, 'tp'), may hold values from -1 to 1
- conv_gain: float32 [1024], P('tp'), may hold values from 0.1 to 1.9
- decay_rate: float32 [64, 64], P('tp'), may hold values from 0.25 to 1
- frequency: float32 [64, 64], P('tp'), may hold values from 0 to 201.06177
- log_step: float32 [64], P('tp'), may hold values from -12 to -2.3
- step_gain: float32 [4, 64, 4096], P('fs', 'tp', 'sp'), may hold values from 0.35 to 2457.6
- drive_matrix: float32 [2, 64, 64, 16], P(None, 'tp'), may hold values from -1 to 1
- read_matrix: float32 [2, 64, 16, 64], P(None, 'tp'), may hold values from -0.5 to 0.5
- skip_gain: float32 [1024], P('tp'), may hold values from -4 to 4
- start_state: float32 [2, 4, 64, 64], P(None, 'fs', 'tp'), may hold values from -6 to 6
- merge_conv: bfloat16 [4096, 1024], P(('sp', 'fs'), 'tp'), may hold values from -0.125 to 0.125
- merge_state: bfloat16 [4096, 1024], P(('sp', 'fs'), 'tp'), may hold values from -0.125 to 0.125
Outputs:
- mixed: bfloat16 [4, 4096, 4096], P('fs', ('sp', 'tp'))
The draws below stay inside these ranges and needn't reach their ends.
All inputs are finite; a program needn't handle non-finite values.
Results may differ from the reference program's by a relative error of at most 0.014.
Values may be sent and summed in bfloat16 or wider, within the bound.
No kernel may reach another device: no remote copies, remote signals or barrier semaphores. Data moves between devices by JAX's collectives and lax.ppermute only.
A program may use at most 128 MiB of HBM per device.

```python
import math
import jax
import jax.numpy as jnp
from jax import lax

D = 4096
CONV_HEADS = 8
HEAD_CH = 128
GROUPS = 64
GROUP_CH = 16
STATE = 64
KERNEL = 31
TOK_DEV = 256
SEQUENCE_COUNT = 4
SEQUENCE_LENGTH = 4096
CONV_CH = 1024
SCAN_CH = 1024
HEAD_BLOCKS = 8


def draw_log_step(key, part):
    ranking = jax.random.permutation(jax.random.fold_in(key, 11), GROUPS)
    slow_count = GROUPS // 2
    slow_mask = ranking < slow_count
    slow_value = jnp.log(jax.random.uniform(jax.random.fold_in(key, 12), (GROUPS,), jnp.float32, 0.2, 0.8) / SEQUENCE_LENGTH)
    fast_value = jnp.log(jax.random.uniform(jax.random.fold_in(key, 13), (GROUPS,), jnp.float32, 0.05, 0.1))
    return jnp.where(slow_mask, slow_value, fast_value).astype(jnp.float32)


def draw_step_gain(key, part):
    block_count = SEQUENCE_LENGTH // TOK_DEV
    per_block = jnp.exp(jax.random.uniform(jax.random.fold_in(key, 21), (SEQUENCE_COUNT, GROUPS, block_count), jnp.float32, math.log(0.5), math.log(2.0)))
    smooth_signal = jnp.repeat(per_block, TOK_DEV, axis=2)
    noisy_signal = jnp.exp(jax.random.uniform(jax.random.fold_in(key, 22), (SEQUENCE_COUNT, GROUPS, SEQUENCE_LENGTH), jnp.float32, math.log(0.7), math.log(1.4)))
    spike_positions = jax.random.randint(jax.random.fold_in(key, 23), (SEQUENCE_COUNT, 3), 0, SEQUENCE_LENGTH)
    position_index = jnp.arange(SEQUENCE_LENGTH, dtype=jnp.int32)
    spike_mask = jnp.any(position_index[None, None, :] == spike_positions[:, :, None], axis=1)
    spike_values = SEQUENCE_LENGTH * jax.random.uniform(jax.random.fold_in(key, 24), (SEQUENCE_COUNT, 1, SEQUENCE_LENGTH), jnp.float32, 0.25, 0.6)
    return jnp.where(spike_mask[:, None, :], spike_values, smooth_signal * noisy_signal).astype(jnp.float32)


def block_scale(rng, dims, pieces, low, top_value):
    def one(dim, shards_of):
        steps = jax.random.uniform(jax.random.fold_in(jax.random.fold_in(rng, 6), dim), (shards_of,), jnp.float32, low / len(pieces), top_value / len(pieces))
        return jnp.repeat(jnp.exp(steps), dims[dim] // shards_of).reshape((-1,) + (1,) * (len(dims) - dim - 1))

    loudness = one(*pieces[0])
    for cut in pieces[1:]:
        loudness = loudness * one(*cut)
    return loudness


def bell_draw(key, extent, deviation, most, split=(), held_as=jnp.bfloat16):
    gain = block_scale(key, extent, split, -0.22, 0.18) if split else 1.0
    result = jax.random.normal(key, extent, jnp.float32) * deviation * gain
    return jnp.minimum(jnp.maximum(result, -most), most).astype(held_as)


def setup_inputs(seed: int = 0) -> dict:
    key_list = jax.random.split(jax.random.key(seed), 18)
    return {
        "stream": bell_draw(key_list[0], (SEQUENCE_COUNT, SEQUENCE_LENGTH, D), 1.0, 6.0, ((0, 4), (1, 16))),
        "norm_gain": jnp.clip(1.0 + 0.18 * jax.random.normal(key_list[1], (D,), jnp.float32), 0.1, 1.9),
        "value_proj": bell_draw(key_list[2], (D, CONV_CH), D ** -0.5, 0.09375, ((0, 64), (1, 8))),
        "gate_proj": bell_draw(key_list[3], (D, CONV_CH), D ** -0.5, 0.09375, ((0, 64), (1, 8))),
        "state_proj": bell_draw(key_list[4], (D, SCAN_CH), D ** -0.5, 0.09375, ((0, 64), (1, 8))),
        "conv_kernel": bell_draw(key_list[5], (KERNEL, CONV_CH), KERNEL ** -0.5, 1.0, ((1, 8),)),
        "conv_gain": jnp.clip(1.0 + 0.18 * jax.random.normal(key_list[6], (CONV_CH,), jnp.float32), 0.1, 1.9),
        "decay_rate": jnp.clip(jnp.exp(math.log(1.0) - 1.3862944 * jax.random.uniform(key_list[7], (GROUPS, STATE), jnp.float32) ** block_scale(key_list[7], (GROUPS, STATE), ((0, 8),), -0.2, 0.2)), 0.25, 1.0),
        "frequency": jnp.clip(201.06177 * jax.random.uniform(key_list[8], (GROUPS, STATE), jnp.float32) ** block_scale(key_list[8], (GROUPS, STATE), ((0, 8),), -0.2, 0.2), 0.0, 201.06177),
        "log_step": draw_log_step(jax.random.fold_in(key_list[17], 71), 0),
        "step_gain": draw_step_gain(jax.random.fold_in(key_list[17], 71), 0),
        "drive_matrix": bell_draw(key_list[11], (2, GROUPS, STATE, GROUP_CH), (2 * GROUP_CH) ** -0.5, 1.0, ((1, 8),), jnp.float32),
        "read_matrix": bell_draw(key_list[12], (2, GROUPS, GROUP_CH, STATE), (2 * STATE) ** -0.5, 0.5, ((1, 8),), jnp.float32),
        "skip_gain": bell_draw(key_list[13], (SCAN_CH,), 1.0, 4.0, ((0, 8),), jnp.float32),
        "start_state": bell_draw(key_list[14], (2, SEQUENCE_COUNT, GROUPS, STATE), 1.0, 6.0, ((1, 4), (2, 8)), jnp.float32),
        "merge_conv": bell_draw(key_list[15], (D, CONV_CH), (CONV_CH + SCAN_CH) ** -0.5, 0.125, ((0, 64), (1, 8))),
        "merge_state": bell_draw(key_list[16], (D, SCAN_CH), (CONV_CH + SCAN_CH) ** -0.5, 0.125, ((0, 64), (1, 8))),
    }


exact_mode = lax.Precision.HIGHEST

def reference(stream, norm_gain, value_proj, gate_proj, state_proj, conv_kernel, conv_gain, decay_rate, frequency, log_step, step_gain, drive_matrix, read_matrix, skip_gain, start_state, merge_conv, merge_state):
    widened = stream.astype(jnp.float32)
    inverse = lax.rsqrt(lax.optimization_barrier(jnp.mean(widened * widened, axis=2, keepdims=True)) + 1e-06)
    normed = (widened * inverse * norm_gain).astype(jnp.bfloat16).reshape(SEQUENCE_COUNT * SEQUENCE_LENGTH, D)
    value_pre = jnp.dot(normed, value_proj, preferred_element_type=jnp.float32)
    gate_pre = jnp.dot(normed, gate_proj, preferred_element_type=jnp.float32)
    gated = (value_pre * jax.nn.sigmoid(gate_pre)).astype(jnp.bfloat16).reshape(SEQUENCE_COUNT, SEQUENCE_LENGTH, CONV_CH)
    scan_input = jnp.dot(normed, state_proj, preferred_element_type=jnp.float32).astype(jnp.bfloat16)
    scan_input = scan_input.reshape(SEQUENCE_COUNT, SEQUENCE_LENGTH, SCAN_CH)
    margin = KERNEL - 1
    padded = jnp.pad(gated, ((0, 0), (margin, 0), (0, 0))).astype(jnp.float32)
    kernel = conv_kernel.astype(jnp.float32)
    mixed_taps = jnp.zeros((SEQUENCE_COUNT, SEQUENCE_LENGTH, CONV_CH), jnp.float32)
    for tap_index in range(KERNEL):
        mixed_taps = mixed_taps + kernel[tap_index] * padded[:, tap_index:tap_index + SEQUENCE_LENGTH]
    grouped = mixed_taps.reshape(SEQUENCE_COUNT, SEQUENCE_LENGTH, CONV_HEADS, HEAD_CH)
    center = grouped - lax.optimization_barrier(jnp.mean(grouped, axis=3, keepdims=True))
    spread = lax.optimization_barrier(jnp.mean(center * center, axis=3, keepdims=True))
    normal = (center * lax.rsqrt(spread + 1e-05)).reshape(SEQUENCE_COUNT, SEQUENCE_LENGTH, CONV_CH) * conv_gain
    conv_out = (normal * jax.nn.sigmoid(normal)).astype(jnp.bfloat16)
    base_step = jnp.exp(log_step)
    magnitude = decay_rate * decay_rate + frequency * frequency

    def advance(carry, inputs):
        state_re, state_im = carry
        gain_now, input_now = inputs
        step_size = (base_step * gain_now)[:, :, None]
        modulus = jnp.exp(-step_size * decay_rate)
        rotation = step_size * frequency
        trans_re = modulus * jnp.cos(rotation)
        trans_im = modulus * jnp.sin(rotation)
        less_re = trans_re - 1.0
        factor_re = (-decay_rate * less_re + frequency * trans_im) / magnitude
        factor_im = (-decay_rate * trans_im - frequency * less_re) / magnitude
        grouped_in = input_now.astype(jnp.float32).reshape(SEQUENCE_COUNT, GROUPS, GROUP_CH)
        drive_re = jnp.einsum('gnc,sgc->sgn', drive_matrix[0], grouped_in, precision=exact_mode)
        drive_im = jnp.einsum('gnc,sgc->sgn', drive_matrix[1], grouped_in, precision=exact_mode)
        push_re = factor_re * drive_re - factor_im * drive_im
        push_im = factor_re * drive_im + factor_im * drive_re
        new_re = trans_re * state_re - trans_im * state_im + push_re
        new_im = trans_re * state_im + trans_im * state_re + push_im
        read_out = jnp.einsum('gcn,sgn->sgc', read_matrix[0], new_re, precision=exact_mode) - jnp.einsum('gcn,sgn->sgc', read_matrix[1], new_im, precision=exact_mode)
        return ((new_re, new_im), read_out)
    gains_by_pos = jnp.transpose(step_gain, (2, 0, 1))
    inputs_by_pos = jnp.transpose(scan_input, (1, 0, 2))
    unused, read_all = lax.scan(advance, (start_state[0], start_state[1]), (gains_by_pos, inputs_by_pos))
    read_all = jnp.transpose(read_all, (1, 0, 2, 3)).reshape(SEQUENCE_COUNT, SEQUENCE_LENGTH, SCAN_CH)
    state_out = jax.nn.gelu(read_all + skip_gain * scan_input.astype(jnp.float32)).astype(jnp.bfloat16)
    conv_rows = conv_out.reshape(SEQUENCE_COUNT * SEQUENCE_LENGTH, CONV_CH)
    state_rows = state_out.reshape(SEQUENCE_COUNT * SEQUENCE_LENGTH, SCAN_CH)
    conv_block = CONV_CH // HEAD_BLOCKS
    scan_block = SCAN_CH // HEAD_BLOCKS
    contract = (((1,), (1,)), ((), ()))
    total = jnp.zeros((SEQUENCE_COUNT * SEQUENCE_LENGTH, D), jnp.float32)
    for block_index in range(HEAD_BLOCKS):
        conv_lo = block_index * conv_block
        scan_lo = block_index * scan_block
        block_sum = lax.dot_general(conv_rows[:, conv_lo:conv_lo + conv_block], merge_conv[:, conv_lo:conv_lo + conv_block], contract, preferred_element_type=jnp.float32)
        block_sum = block_sum + lax.dot_general(state_rows[:, scan_lo:scan_lo + scan_block], merge_state[:, scan_lo:scan_lo + scan_block], contract, preferred_element_type=jnp.float32)
        rounded = lax.optimization_barrier(block_sum.astype(jnp.bfloat16))
        total = total + rounded.astype(jnp.float32)
    return total.astype(jnp.bfloat16).reshape(SEQUENCE_COUNT, SEQUENCE_LENGTH, D)
```

```python
import functools

import jax
import jax.numpy as jnp
from jax import lax
from jax.experimental import pallas as pl
from jax.experimental.pallas import tpu as pltpu
from jax.sharding import PartitionSpec as P

LANES = 128
CHUNKS = 8


def shifted(array, axis, by):
    devices = lax.axis_size(axis)
    return lax.ppermute(array, axis, [(i, (i + by) % devices) for i in range(devices)])


def block_diagonal(blocks):
    g, a, b = blocks.shape
    spread = blocks[:, :, None, :] * jnp.eye(g, dtype=blocks.dtype)[:, None, :, None]
    return spread.reshape(g * a, g * b)


def norm_kernel(before, stream, gain, out):
    lead = before.shape[0]

    def normed(block):
        widened = block.astype(jnp.float32)
        inverse = lax.rsqrt(jnp.mean(widened * widened, axis=1, keepdims=True) + 1e-06)
        return (widened * inverse * gain[...]).astype(jnp.bfloat16)

    out[:lead, :] = normed(before[...])

    def step(i, _):
        at = pl.multiple_of(i * lead, lead)
        out[pl.ds(pl.multiple_of(at + lead, lead), lead), :] = normed(stream[pl.ds(at, lead), :])
        return 0

    lax.fori_loop(0, stream.shape[0] // lead, step, 0)


def scan_kernel(devices, sharers, part, index, normed, read_re, read_im, *refs):
    pieces = refs[:sharers]
    (trans_re, trans_im, factor_re, factor_im, drive_re, drive_im) = refs[sharers : sharers + 6]
    scan_input, read_local, whole_re, whole_im, sent = refs[sharers + 6 : sharers + 11]
    weights, push_re, push_im, run_re, run_im, prod_re, prod_im = refs[sharers + 11 :]
    sharer = index[1]
    for j in range(sharers):
        y = lax.rem(sharer - j + sharers, sharers)
        for z in range(devices):
            at = pl.multiple_of(z * sharers * part + y * part, part)
            weights[pl.ds(at, part), :] = pieces[j][z * part : (z + 1) * part, :]
    tiles, count, _ = trans_re.shape
    lead = normed.shape[0] - count
    pre = jnp.dot(normed[lead:, :], weights[...], preferred_element_type=jnp.float32)
    inputs = pre.astype(jnp.bfloat16)
    scan_input[...] = inputs
    for j in range(tiles):
        lanes = slice(j * LANES, (j + 1) * LANES)
        d_re = jnp.dot(inputs, drive_re[:, lanes], preferred_element_type=jnp.float32)
        d_im = jnp.dot(inputs, drive_im[:, lanes], preferred_element_type=jnp.float32)
        f_re, f_im = factor_re[j], factor_im[j]
        push_re[j] = f_re * d_re - f_im * d_im
        push_im[j] = f_re * d_im + f_im * d_re
    length = count // CHUNKS

    def step(i, carry):
        out = []
        for j in range(tiles):
            s_re, s_im, p_re, p_im = carry[j]
            at = pl.ds(i, CHUNKS, stride=length)
            a_re, a_im = trans_re[j, at, :], trans_im[j, at, :]
            n_re = a_re * s_re - a_im * s_im + push_re[j, at, :]
            n_im = a_re * s_im + a_im * s_re + push_im[j, at, :]
            q_re = a_re * p_re - a_im * p_im
            q_im = a_re * p_im + a_im * p_re
            run_re[j, at, :] = n_re
            run_im[j, at, :] = n_im
            prod_re[j, at, :] = q_re
            prod_im[j, at, :] = q_im
            out.append((n_re, n_im, q_re, q_im))
        return tuple(out)

    zero = jnp.zeros((CHUNKS, LANES), jnp.float32)
    one = jnp.ones((CHUNKS, LANES), jnp.float32)
    last = lax.fori_loop(0, length, step, tuple((zero, zero, one, zero) for _ in range(tiles)))
    total = [[], [], [], []]
    read = jnp.zeros((count, LANES), jnp.float32)
    for j in range(tiles):
        s_re, s_im, p_re, p_im = last[j]
        a_re, a_im = one[0:1], zero[0:1]
        b_re, b_im = zero[0:1], zero[0:1]
        states_re, states_im = [], []
        for c in range(CHUNKS):
            at = slice(c * length, (c + 1) * length)
            q_re, q_im = prod_re[j, at, :], prod_im[j, at, :]
            states_re.append((run_re[j, at, :] + q_re * b_re - q_im * b_im).astype(jnp.bfloat16))
            states_im.append((run_im[j, at, :] + q_re * b_im + q_im * b_re).astype(jnp.bfloat16))
            whole_re[j, at, :] = (q_re * a_re - q_im * a_im).astype(jnp.bfloat16)
            whole_im[j, at, :] = (q_re * a_im + q_im * a_re).astype(jnp.bfloat16)
            k_re, k_im = p_re[c : c + 1], p_im[c : c + 1]
            b_re, b_im = (
                k_re * b_re - k_im * b_im + s_re[c : c + 1],
                k_re * b_im + k_im * b_re + s_im[c : c + 1],
            )
            a_re, a_im = k_re * a_re - k_im * a_im, k_re * a_im + k_im * a_re
        lanes = slice(j * LANES, (j + 1) * LANES)
        read = read + jnp.dot(jnp.concatenate(states_re, axis=0), read_re[lanes, :], preferred_element_type=jnp.float32)
        read = read - jnp.dot(jnp.concatenate(states_im, axis=0), read_im[lanes, :], preferred_element_type=jnp.float32)
        for kind, row in enumerate((a_re, a_im, b_re, b_im)):
            total[kind].append(row)
    read_local[...] = read
    table = jnp.concatenate([row for kind in total for row in kind], axis=0)
    for r in range(devices):
        sent[r] = table


def state_kernel(devices, index, arrived, whole_re, whole_im, read_local, start, read_re, read_im, skip, scan_input, out):
    me = index[0]
    tiles = whole_re.shape[0]
    e_re, e_im = start[0:tiles], start[tiles:]
    for z in range(devices - 1):
        a_re, a_im = arrived[z, 0:tiles, :], arrived[z, tiles : 2 * tiles, :]
        b_re, b_im = arrived[z, 2 * tiles : 3 * tiles, :], arrived[z, 3 * tiles :, :]
        n_re = a_re * e_re - a_im * e_im + b_re
        n_im = a_re * e_im + a_im * e_re + b_im
        before = z < me
        e_re, e_im = jnp.where(before, n_re, e_re), jnp.where(before, n_im, e_im)
    read = read_local[...] + skip[...] * scan_input[...].astype(jnp.float32)
    for j in range(tiles):
        p_re, p_im = whole_re[j].astype(jnp.float32), whole_im[j].astype(jnp.float32)
        x_re, x_im = e_re[j : j + 1], e_im[j : j + 1]
        lanes = slice(j * LANES, (j + 1) * LANES)
        late_re = (p_re * x_re - p_im * x_im).astype(jnp.bfloat16)
        late_im = (p_re * x_im + p_im * x_re).astype(jnp.bfloat16)
        read = read + jnp.dot(late_re, read_re[lanes, :], preferred_element_type=jnp.float32)
        read = read - jnp.dot(late_im, read_im[lanes, :], preferred_element_type=jnp.float32)
    out[...] = jax.nn.gelu(read).astype(jnp.bfloat16)


def merge_kernel(taps, index, normed, weights, kernel, gain, state_out, mine, other, padded, rows_in, rows_by_slot):
    seat = index[2]
    pre = jnp.dot(normed[...], weights[:, : 2 * LANES], preferred_element_type=jnp.float32)
    gated = (pre[:, :LANES] * jax.nn.sigmoid(pre[:, LANES:])).astype(jnp.bfloat16)
    padded[...] = gated.astype(jnp.float32)
    count = state_out.shape[0]
    first = padded.shape[0] - count - (taps - 1)
    by_tap = kernel[...].astype(jnp.float32)
    acc = by_tap[0:1] * padded[first : first + count, :]
    for k in range(1, taps):
        acc = acc + by_tap[k : k + 1] * padded[first + k : first + k + count, :]
    center = acc - jnp.mean(acc, axis=1, keepdims=True)
    spread = jnp.mean(center * center, axis=1, keepdims=True)
    normal = center * lax.rsqrt(spread + 1e-05) * gain[...]
    rows_in[:, :LANES] = (normal * jax.nn.sigmoid(normal)).astype(jnp.bfloat16)
    rows_in[:, LANES:] = state_out[...]
    seats = 4
    slot = count // (2 * seats)
    core, chip = lax.rem(seat, 2), lax.div(seat, 2)
    for half in range(2):
        wanted = core if half == 0 else 1 - core
        for d in range(seats):
            source = lax.rem(chip + d, seats) * 2 + wanted
            to = (half * seats + d) * slot
            rows_by_slot[to : to + slot, :] = rows_in[pl.ds(pl.multiple_of(source * slot, slot), slot), :]
    lhs = rows_by_slot[...]
    wide = 512
    for f in range(weights.shape[0] // wide):
        at = slice(f * wide, (f + 1) * wide)
        block = lax.dot_general(lhs, weights[at, 2 * LANES :], (((1,), (1,)), ((), ())), preferred_element_type=jnp.float32).astype(jnp.bfloat16)
        mine[:, at] = block[: count // 2]
        other[:, at] = block[count // 2 :]


def call(kernel, mib, out_shapes, scratch, *args):
    in_specs = [pl.BlockSpec(memory_space=pltpu.SMEM if a.dtype == jnp.int32 else pltpu.VMEM) for a in args]
    return pl.pallas_call(
        kernel,
        out_shape=[jax.ShapeDtypeStruct(*s) for s in out_shapes],
        in_specs=in_specs,
        out_specs=[pl.BlockSpec(memory_space=pltpu.VMEM) for _ in out_shapes],
        scratch_shapes=[pltpu.VMEM(*s) for s in scratch],
        compiler_params=pltpu.CompilerParams(vmem_limit_bytes=mib * 1024 * 1024),
    )(*args)


def body(stream, norm_gain, value_proj, gate_proj, state_proj, conv_kernel, conv_gain, decay_rate, frequency, log_step, step_gain, drive_matrix, read_matrix, skip_gain, start_state, merge_conv, merge_state):
    f32, bf16 = jnp.float32, jnp.bfloat16
    rows, width = stream.shape[1:]
    part = value_proj.shape[0]
    devices, sharers = lax.axis_size("sp"), lax.axis_size("fs")
    index = jnp.stack([lax.axis_index(a) for a in ("sp", "fs", "tp")]).astype(jnp.int32)

    near = lax.all_gather(jnp.concatenate([value_proj, gate_proj, merge_conv, merge_state], axis=1), "fs", axis=0, tiled=True)
    weights = lax.all_gather(near, "sp", axis=0, tiled=True)
    column = lax.all_gather(state_proj, "sp", axis=0, tiled=True)
    pieces = [column] + [shifted(column, "fs", j) for j in range(1, sharers)]

    lead = 32
    tail = lax.ppermute(stream[0, rows - lead :], "sp", [(i, i + 1) for i in range(devices - 1)])
    (normed,) = call(norm_kernel, 10, [((rows + lead, width), bf16)], [], tail, stream[0], norm_gain[None])

    group_count, state_size = decay_rate.shape
    flat = group_count * state_size
    tiles = flat // LANES
    step = jnp.exp(log_step)[:, None] * step_gain[0]
    per = group_count // tiles
    step = jnp.transpose(step.reshape(tiles, per, rows), (0, 2, 1))[..., None]
    step = lax.optimization_barrier(jnp.broadcast_to(step, (tiles, rows, per, state_size)).reshape(tiles, rows, LANES))
    rate = decay_rate.reshape(tiles, 1, LANES)
    turn = frequency.reshape(tiles, 1, LANES)
    modulus = jnp.exp(-step * rate)
    rotation = step * turn
    trans_re = modulus * jnp.cos(rotation)
    trans_im = modulus * jnp.sin(rotation)
    magnitude = rate * rate + turn * turn
    less_re = trans_re - 1.0
    factor_re = (-rate * less_re + turn * trans_im) / magnitude
    factor_im = (-rate * trans_im - turn * less_re) / magnitude
    drive = [block_diagonal(jnp.transpose(drive_matrix[i], (0, 2, 1)).astype(bf16)) for i in range(2)]
    read = [block_diagonal(jnp.transpose(read_matrix[i], (0, 2, 1)).astype(bf16)) for i in range(2)]
    start = start_state[:, 0].reshape(2 * tiles, LANES)

    big = ((tiles, rows, LANES), f32)
    slim = ((tiles, rows, LANES), bf16)
    scan_input, read_local, whole_re, whole_im, sent = call(
        functools.partial(scan_kernel, devices, sharers, part),
        20,
        [((rows, LANES), bf16), ((rows, LANES), f32), slim, slim, ((devices, 4 * tiles, LANES), f32)],
        [((width, LANES), bf16), big, big, big, big, big, big],
        index, normed, *read, *pieces, trans_re, trans_im, factor_re, factor_im, *drive,
    )
    arrived = lax.all_to_all(sent, "sp", split_axis=0, concat_axis=0, tiled=True)
    (state_out,) = call(
        functools.partial(state_kernel, devices),
        8,
        [((rows, LANES), bf16)],
        [],
        index, arrived, whole_re, whole_im, read_local, start, *read, skip_gain[None], scan_input,
    )
    mine, other = call(
        functools.partial(merge_kernel, conv_kernel.shape[0]),
        16,
        [((rows // 2, width), bf16)] * 2,
        [((rows + lead, LANES), f32), ((rows, 2 * LANES), bf16), ((rows, 2 * LANES), bf16)],
        index, normed, weights, conv_kernel, conv_gain[None], state_out,
    )
    got = lax.ppermute(other, "tp", [(i, i ^ 1) for i in range(8)])
    both = (mine.astype(f32) + got.astype(f32)).astype(bf16)
    slot = rows // 8
    mixed = both[:slot].astype(f32)
    for d in range(1, 4):
        mixed = mixed + shifted(both[d * slot : (d + 1) * slot], "tp", 2 * d).astype(f32)
    return mixed.astype(bf16)[None]


def solution(mesh):
    return jax.shard_map(
        body,
        mesh=mesh,
        in_specs=(
            P("fs", "sp", None),
            P(),
            P(("sp", "fs"), "tp"),
            P(("sp", "fs"), "tp"),
            P(("sp", "fs"), "tp"),
            P(None, "tp"),
            P("tp"),
            P("tp", None),
            P("tp", None),
            P("tp"),
            P("fs", "tp", "sp"),
            P(None, "tp", None, None),
            P(None, "tp", None, None),
            P("tp"),
            P(None, "fs", "tp", None),
            P(("sp", "fs"), "tp"),
            P(("sp", "fs"), "tp"),
        ),
        out_specs=P("fs", ("sp", "tp"), None),
        check_vma=False,
    )
```

```python
import functools

import jax
import jax.numpy as jnp
from jax import lax
from jax.experimental import pallas as pl
from jax.experimental.pallas import tpu as pltpu
from jax.sharding import PartitionSpec as P

LANES = 128
CHUNKS = 8


def shifted(array, axis, by):
    devices = lax.axis_size(axis)
    return lax.ppermute(array, axis, [(i, (i + by) % devices) for i in range(devices)])


def from_everyone(array, axis):
    copies = jnp.broadcast_to(array, (lax.axis_size(axis), *array.shape))
    return lax.all_to_all(copies, axis, split_axis=0, concat_axis=0, tiled=True)


def block_diagonal(blocks):
    g, a, b = blocks.shape
    spread = blocks[:, :, None, :] * jnp.eye(g, dtype=blocks.dtype)[:, None, :, None]
    return spread.reshape(g * a, g * b)


def spread_kernel(rates, turns, logs, gains, step, rate, turn):
    groups, size = rates.shape
    per = LANES // size
    by_row = jnp.transpose(jnp.exp(logs[...]) * gains[...])
    lane = lax.broadcasted_iota(jnp.int32, (by_row.shape[0], LANES), 1)
    for j in range(groups // per):
        wide = jnp.broadcast_to(by_row[:, j * per : j * per + 1], lane.shape)
        for k in range(1, per):
            at = j * per + k
            wide = jnp.where(lane < k * size, wide, jnp.broadcast_to(by_row[:, at : at + 1], lane.shape))
        step[j] = wide
        for row, out in ((rates, rate), (turns, turn)):
            out[j] = jnp.concatenate([row[j * per + k : j * per + k + 1, :] for k in range(per)], axis=1)


def norm_kernel(stream, gain, out, tail):
    block = tail.shape[0]

    def step(i, _):
        at = pl.ds(pl.multiple_of(i * block, block), block)
        widened = stream[at, :].astype(jnp.float32)
        inverse = lax.rsqrt(jnp.mean(widened * widened, axis=1, keepdims=True) + 1e-06)
        out[at, :] = (widened * inverse * gain[...]).astype(jnp.bfloat16)
        return 0

    lax.fori_loop(0, stream.shape[0] // block, step, 0)
    tail[...] = out[stream.shape[0] - block :, :]


def scan_kernel(devices, sharers, part, index, normed, read_re, read_im, skip, *refs):
    pieces = refs[:sharers]
    (trans_re, trans_im, factor_re, factor_im, drive_re, drive_im) = refs[sharers : sharers + 6]
    outs = refs[sharers + 6 : sharers + 9]
    weights, push_re, push_im, run_re, run_im, prod_re, prod_im, read_local, whole, sent, sems = refs[sharers + 9 :]
    leaving = [pltpu.make_async_copy(a, b, sems.at[k]) for k, (a, b) in enumerate(zip((read_local, whole, sent), outs))]
    sharer = index[1]
    for j in range(sharers):
        y = lax.rem(sharer - j + sharers, sharers)
        for z in range(devices):
            at = pl.multiple_of(z * sharers * part + y * part, part)
            weights[pl.ds(at, part), :] = pieces[j][z * part : (z + 1) * part, :]
    tiles, count, _ = trans_re.shape
    pre = jnp.dot(normed[...], weights[...], preferred_element_type=jnp.float32)
    inputs = pre.astype(jnp.bfloat16)
    for j in range(tiles):
        lanes = slice(j * LANES, (j + 1) * LANES)
        d_re = jnp.dot(inputs, drive_re[:, lanes], preferred_element_type=jnp.float32)
        d_im = jnp.dot(inputs, drive_im[:, lanes], preferred_element_type=jnp.float32)
        f_re, f_im = factor_re[j], factor_im[j]
        push_re[j] = f_re * d_re - f_im * d_im
        push_im[j] = f_re * d_im + f_im * d_re
    length = count // CHUNKS

    def step(i, carry):
        out = []
        for j in range(tiles):
            s_re, s_im, p_re, p_im = carry[j]
            at = pl.ds(i, CHUNKS, stride=length)
            a_re, a_im = trans_re[j, at, :], trans_im[j, at, :]
            n_re = a_re * s_re - a_im * s_im + push_re[j, at, :]
            n_im = a_re * s_im + a_im * s_re + push_im[j, at, :]
            q_re = a_re * p_re - a_im * p_im
            q_im = a_re * p_im + a_im * p_re
            run_re[j, at, :] = n_re
            run_im[j, at, :] = n_im
            prod_re[j, at, :] = q_re
            prod_im[j, at, :] = q_im
            out.append((n_re, n_im, q_re, q_im))
        return tuple(out)

    zero = jnp.zeros((CHUNKS, LANES), jnp.float32)
    one = jnp.ones((CHUNKS, LANES), jnp.float32)
    last = lax.fori_loop(0, length, step, tuple((zero, zero, one, zero) for _ in range(tiles)))
    total = [[], [], [], []]
    read = skip[...] * inputs.astype(jnp.float32)
    for j in range(tiles):
        s_re, s_im, p_re, p_im = last[j]
        a_re, a_im = one[0:1], zero[0:1]
        b_re, b_im = zero[0:1], zero[0:1]
        states_re, states_im = [], []
        for c in range(CHUNKS):
            at = slice(c * length, (c + 1) * length)
            q_re, q_im = prod_re[j, at, :], prod_im[j, at, :]
            states_re.append((run_re[j, at, :] + q_re * b_re - q_im * b_im).astype(jnp.bfloat16))
            states_im.append((run_im[j, at, :] + q_re * b_im + q_im * b_re).astype(jnp.bfloat16))
            whole[0, j, at, :] = (q_re * a_re - q_im * a_im).astype(jnp.bfloat16)
            whole[1, j, at, :] = (q_re * a_im + q_im * a_re).astype(jnp.bfloat16)
            k_re, k_im = p_re[c : c + 1], p_im[c : c + 1]
            b_re, b_im = (
                k_re * b_re - k_im * b_im + s_re[c : c + 1],
                k_re * b_im + k_im * b_re + s_im[c : c + 1],
            )
            a_re, a_im = k_re * a_re - k_im * a_im, k_re * a_im + k_im * a_re
        lanes = slice(j * LANES, (j + 1) * LANES)
        read = read + jnp.dot(jnp.concatenate(states_re, axis=0), read_re[lanes, :], preferred_element_type=jnp.float32)
        read = read - jnp.dot(jnp.concatenate(states_im, axis=0), read_im[lanes, :], preferred_element_type=jnp.float32)
        for kind, row in enumerate((a_re, a_im, b_re, b_im)):
            total[kind].append(row)
    read_local[...] = read
    leaving[0].start()
    leaving[1].start()
    table = jnp.concatenate([row for kind in total for row in kind], axis=0)
    for r in range(devices):
        sent[r] = table
    leaving[2].start()
    for copy in leaving:
        copy.wait()


def state_kernel(devices, index, arrived_out, whole_out, read_out, start, read_re, read_im, out, arrived, whole, read_local, sems):
    me = index[0]
    tiles = whole.shape[1]
    coming = [
        pltpu.make_async_copy(a, b, sems.at[k])
        for k, (a, b) in enumerate(((arrived_out, arrived), (whole_out, whole), (read_out, read_local)))
    ]
    for copy in coming:
        copy.start()
    for copy in coming:
        copy.wait()
    e_re, e_im = start[0:tiles], start[tiles:]
    for z in range(devices - 1):
        a_re, a_im = arrived[z, 0:tiles, :], arrived[z, tiles : 2 * tiles, :]
        b_re, b_im = arrived[z, 2 * tiles : 3 * tiles, :], arrived[z, 3 * tiles :, :]
        n_re = a_re * e_re - a_im * e_im + b_re
        n_im = a_re * e_im + a_im * e_re + b_im
        before = z < me
        e_re, e_im = jnp.where(before, n_re, e_re), jnp.where(before, n_im, e_im)
    read = read_local[...]
    for j in range(tiles):
        p_re, p_im = whole[0, j].astype(jnp.float32), whole[1, j].astype(jnp.float32)
        x_re, x_im = e_re[j : j + 1], e_im[j : j + 1]
        lanes = slice(j * LANES, (j + 1) * LANES)
        late_re = (p_re * x_re - p_im * x_im).astype(jnp.bfloat16)
        late_im = (p_re * x_im + p_im * x_re).astype(jnp.bfloat16)
        read = read + jnp.dot(late_re, read_re[lanes, :], preferred_element_type=jnp.float32)
        read = read - jnp.dot(late_im, read_im[lanes, :], preferred_element_type=jnp.float32)
    out[...] = jax.nn.gelu(read).astype(jnp.bfloat16)


def merge_kernel(taps, index, before, normed, weights, kernel, gain, state_out, mine, other, rows, gates, merges, padded, rows_in, rows_by_slot, kernel_in, gain_in, sems, small):
    seat = index[2]
    pieces = sems.shape[0] // 2
    high = gates.shape[0] // pieces

    def fetch(to, column, k, sem):
        at = pl.ds(k * high, high)
        return pltpu.make_async_copy(weights.at[at, pl.ds(column * 2 * LANES, 2 * LANES)], to.at[at, :], sems.at[sem])

    for k in range(pieces):
        fetch(gates, 0, k, k).start()
    for k in range(pieces):
        fetch(merges, 1, k, pieces + k).start()
    tiny = [pltpu.make_async_copy(a, b, small.at[k]) for k, (a, b) in enumerate(((kernel, kernel_in), (gain, gain_in)))]
    for copy in tiny:
        copy.start()
    lead = before.shape[0]
    rows[:lead, :] = before[...]
    rows[lead:, :] = normed[...]
    pre = jnp.zeros((rows.shape[0], 2 * LANES), jnp.float32)
    for k in range(pieces):
        fetch(gates, 0, k, k).wait()
        at = slice(k * high, (k + 1) * high)
        pre = pre + jnp.dot(rows[:, at], gates[at, :], preferred_element_type=jnp.float32)
    gated = (pre[:, :LANES] * jax.nn.sigmoid(pre[:, LANES:])).astype(jnp.bfloat16)
    padded[...] = gated.astype(jnp.float32)
    count = state_out.shape[0]
    first = padded.shape[0] - count - (taps - 1)
    for copy in tiny:
        copy.wait()
    by_tap = kernel_in[...].astype(jnp.float32)
    acc = by_tap[0:1] * padded[first : first + count, :]
    for k in range(1, taps):
        acc = acc + by_tap[k : k + 1] * padded[first + k : first + k + count, :]
    center = acc - jnp.mean(acc, axis=1, keepdims=True)
    spread = jnp.mean(center * center, axis=1, keepdims=True)
    normal = center * lax.rsqrt(spread + 1e-05) * gain_in[...]
    rows_in[:, :LANES] = (normal * jax.nn.sigmoid(normal)).astype(jnp.bfloat16)
    rows_in[:, LANES:] = state_out[...]
    seats = 4
    slot = count // (2 * seats)
    core, chip = lax.rem(seat, 2), lax.div(seat, 2)
    for half in range(2):
        wanted = core if half == 0 else 1 - core
        for d in range(seats):
            source = lax.rem(chip + d, seats) * 2 + wanted
            to = (half * seats + d) * slot
            rows_by_slot[to : to + slot, :] = rows_in[pl.ds(pl.multiple_of(source * slot, slot), slot), :]
    lhs = rows_by_slot[...]
    for k in range(pieces):
        fetch(merges, 1, k, pieces + k).wait()
    wide = 512
    for f in range(merges.shape[0] // wide):
        at = slice(f * wide, (f + 1) * wide)
        block = lax.dot_general(lhs, merges[at, :], (((1,), (1,)), ((), ())), preferred_element_type=jnp.float32).astype(jnp.bfloat16)
        mine[:, at] = block[: count // 2]
        other[:, at] = block[count // 2 :]


def call(kernel, mib, out_shapes, scratch, *args, left=(), kept=False):
    def spec(k, a):
        space = pltpu.SMEM if a.dtype == jnp.int32 else pltpu.HBM if k in left else pltpu.VMEM
        return pl.BlockSpec(memory_space=space)

    return pl.pallas_call(
        kernel,
        out_shape=[jax.ShapeDtypeStruct(*s) for s in out_shapes],
        in_specs=[spec(k, a) for k, a in enumerate(args)],
        out_specs=[pl.BlockSpec(memory_space=pltpu.HBM if kept else pltpu.VMEM) for _ in out_shapes],
        scratch_shapes=[pltpu.VMEM(*s) if isinstance(s, tuple) else s for s in scratch],
        compiler_params=pltpu.CompilerParams(vmem_limit_bytes=mib * 1024 * 1024),
    )(*args)


def body(stream, norm_gain, value_proj, gate_proj, state_proj, conv_kernel, conv_gain, decay_rate, frequency, log_step, step_gain, drive_matrix, read_matrix, skip_gain, start_state, merge_conv, merge_state):
    f32, bf16 = jnp.float32, jnp.bfloat16
    rows, width = stream.shape[1:]
    part = value_proj.shape[0]
    devices, sharers = lax.axis_size("sp"), lax.axis_size("fs")
    index = jnp.stack([lax.axis_index(a) for a in ("sp", "fs", "tp")]).astype(jnp.int32)

    near = from_everyone(jnp.concatenate([value_proj, gate_proj, merge_conv, merge_state], axis=1), "fs")
    near = near.reshape(sharers * part, 4 * LANES)
    near, state_proj = lax.optimization_barrier((near, state_proj))
    weights = lax.all_gather(near, "sp", axis=0, tiled=True)
    column = lax.all_gather(state_proj, "sp", axis=0, tiled=True)
    group_count, state_size = decay_rate.shape
    flat = group_count * state_size
    tiles = flat // LANES
    small = ((tiles, 1, LANES), f32)
    step, rate, turn = call(
        spread_kernel, 4, [((tiles, rows, LANES), f32), small, small], [],
        decay_rate, frequency, log_step[:, None], step_gain[0],
    )
    tokens = stream[0]
    step, tokens, column = lax.optimization_barrier((step, tokens, column))
    pieces = [column] + [shifted(column, "fs", j) for j in range(1, sharers)]
    lead = 32
    normed, tail = call(norm_kernel, 10, [((rows, width), bf16), ((lead, width), bf16)], [], tokens, norm_gain[None])

    modulus = jnp.exp(-step * rate)
    rotation = step * turn
    trans_re = modulus * jnp.cos(rotation)
    trans_im = modulus * jnp.sin(rotation)
    magnitude = rate * rate + turn * turn
    less_re = trans_re - 1.0
    factor_re = (-rate * less_re + turn * trans_im) / magnitude
    factor_im = (-rate * trans_im - turn * less_re) / magnitude
    drive = [block_diagonal(jnp.transpose(drive_matrix[i], (0, 2, 1)).astype(bf16)) for i in range(2)]
    read = [block_diagonal(jnp.transpose(read_matrix[i], (0, 2, 1)).astype(bf16)) for i in range(2)]
    start = start_state[:, 0].reshape(2 * tiles, LANES)

    big = ((tiles, rows, LANES), f32)
    outs = [((rows, LANES), f32), ((2, tiles, rows, LANES), bf16), ((devices, 4 * tiles, LANES), f32)]
    read_local, whole, sent = call(
        functools.partial(scan_kernel, devices, sharers, part),
        20,
        outs,
        [((width, LANES), bf16), big, big, big, big, big, big, *outs, pltpu.SemaphoreType.DMA((3,))],
        index, normed, *read, skip_gain[None], *pieces, trans_re, trans_im, factor_re, factor_im, *drive,
        kept=True,
    )
    sent, tail = lax.optimization_barrier((sent, tail))
    arrived = lax.all_to_all(sent, "sp", split_axis=0, concat_axis=0, tiled=True)
    before = lax.ppermute(tail, "sp", [(i, i + 1) for i in range(devices - 1)])
    (state_out,) = call(
        functools.partial(state_kernel, devices),
        8,
        [((rows, LANES), bf16)],
        [outs[2], outs[1], outs[0], pltpu.SemaphoreType.DMA((3,))],
        index, arrived, whole, read_local, start, *read,
        left=(1, 2, 3),
    )
    copies = 4
    mine, other = call(
        functools.partial(merge_kernel, conv_kernel.shape[0]),
        24,
        [((rows // 2, width), bf16)] * 2,
        [
            ((rows + lead, width), bf16),
            ((width, 2 * LANES), bf16),
            ((width, 2 * LANES), bf16),
            ((rows + lead, LANES), f32),
            ((rows, 2 * LANES), bf16),
            ((rows, 2 * LANES), bf16),
            (conv_kernel.shape, bf16),
            ((1, LANES), f32),
            pltpu.SemaphoreType.DMA((2 * copies,)),
            pltpu.SemaphoreType.DMA((2,)),
        ],
        index, before, normed, pltpu.with_memory_space_constraint(weights, pltpu.HBM), conv_kernel, conv_gain[None], state_out,
        left=(3, 4, 5),
    )
    got = lax.ppermute(other, "tp", [(i, i ^ 1) for i in range(8)])
    both = (mine.astype(f32) + got.astype(f32)).astype(bf16)
    slot = rows // 8
    mixed = both[:slot].astype(f32)
    for d in range(1, 4):
        mixed = mixed + shifted(both[d * slot : (d + 1) * slot], "tp", 2 * d).astype(f32)
    return mixed.astype(bf16)[None]


def solution(mesh):
    return jax.shard_map(
        body,
        mesh=mesh,
        in_specs=(
            P("fs", "sp", None),
            P(),
            P(("sp", "fs"), "tp"),
            P(("sp", "fs"), "tp"),
            P(("sp", "fs"), "tp"),
            P(None, "tp"),
            P("tp"),
            P("tp", None),
            P("tp", None),
            P("tp"),
            P("fs", "tp", "sp"),
            P(None, "tp", None, None),
            P(None, "tp", None, None),
            P("tp"),
            P(None, "fs", "tp", None),
            P(("sp", "fs"), "tp"),
            P(("sp", "fs"), "tp"),
        ),
        out_specs=P("fs", ("sp", "tp"), None),
        check_vma=False,
    )
```

```python
import functools

import jax
import jax.numpy as jnp
from jax import lax
from jax.experimental import pallas as pl
from jax.experimental.pallas import tpu as pltpu
from jax.sharding import PartitionSpec as P


LANES = 128
CHUNKS = 8


def shifted(array, axis, by):
    devices = lax.axis_size(axis)
    return lax.ppermute(array, axis, [(i, (i + by) % devices) for i in range(devices)])


def from_everyone(array, axis):
    copies = jnp.broadcast_to(array, (lax.axis_size(axis), *array.shape))
    return lax.all_to_all(copies, axis, split_axis=0, concat_axis=0, tiled=True)


def block_diagonal(blocks):
    g, a, b = blocks.shape
    spread = blocks[:, :, None, :] * jnp.eye(g, dtype=blocks.dtype)[:, None, :, None]
    return spread.reshape(g * a, g * b)


def spread_kernel(rates, turns, logs, gains, step, rate, turn):
    groups, size = rates.shape
    per = LANES // size
    by_row = jnp.transpose(jnp.exp(logs[...]) * gains[...])
    lane = lax.broadcasted_iota(jnp.int32, (by_row.shape[0], LANES), 1)
    for j in range(groups // per):
        wide = jnp.broadcast_to(by_row[:, j * per : j * per + 1], lane.shape)
        for k in range(1, per):
            at = j * per + k
            wide = jnp.where(lane < k * size, wide, jnp.broadcast_to(by_row[:, at : at + 1], lane.shape))
        step[j] = wide
        for row, out in ((rates, rate), (turns, turn)):
            out[j] = jnp.concatenate([row[j * per + k : j * per + k + 1, :] for k in range(per)], axis=1)


def norm_kernel(stream, gain, out, tail):
    block = tail.shape[0]

    def step(i, _):
        at = pl.ds(pl.multiple_of(i * block, block), block)
        widened = stream[at, :].astype(jnp.float32)
        inverse = lax.rsqrt(jnp.mean(widened * widened, axis=1, keepdims=True) + 1e-06)
        out[at, :] = (widened * inverse * gain[...]).astype(jnp.bfloat16)
        return 0

    lax.fori_loop(0, stream.shape[0] // block, step, 0)
    tail[...] = out[stream.shape[0] - block :, :]


def scan_kernel(devices, sharers, part, index, normed, read_re, read_im, skip, *refs):
    pieces = refs[:sharers]
    (trans_re, trans_im, factor_re, factor_im, drive_re, drive_im) = refs[sharers : sharers + 6]
    outs = refs[sharers + 6 : sharers + 9]
    weights, push_re, push_im, run_re, run_im, prod_re, prod_im, read_local, whole, sent, sems = refs[sharers + 9 :]
    leaving = [pltpu.make_async_copy(a, b, sems.at[k]) for k, (a, b) in enumerate(zip((read_local, whole, sent), outs))]
    sharer = index[1]
    for j in range(sharers):
        y = lax.rem(sharer - j + sharers, sharers)
        for z in range(devices):
            at = pl.multiple_of(z * sharers * part + y * part, part)
            weights[pl.ds(at, part), :] = pieces[j][z * part : (z + 1) * part, :]
    tiles, count, _ = trans_re.shape
    pre = jnp.dot(normed[...], weights[...], preferred_element_type=jnp.float32)
    inputs = pre.astype(jnp.bfloat16)
    for j in range(tiles):
        lanes = slice(j * LANES, (j + 1) * LANES)
        d_re = jnp.dot(inputs, drive_re[:, lanes], preferred_element_type=jnp.float32)
        d_im = jnp.dot(inputs, drive_im[:, lanes], preferred_element_type=jnp.float32)
        f_re, f_im = factor_re[j], factor_im[j]
        push_re[j] = f_re * d_re - f_im * d_im
        push_im[j] = f_re * d_im + f_im * d_re
    length = count // CHUNKS

    def step(i, carry):
        out = []
        for j in range(tiles):
            s_re, s_im, p_re, p_im = carry[j]
            at = pl.ds(i, CHUNKS, stride=length)
            a_re, a_im = trans_re[j, at, :], trans_im[j, at, :]
            n_re = a_re * s_re - a_im * s_im + push_re[j, at, :]
            n_im = a_re * s_im + a_im * s_re + push_im[j, at, :]
            q_re = a_re * p_re - a_im * p_im
            q_im = a_re * p_im + a_im * p_re
            run_re[j, at, :] = n_re
            run_im[j, at, :] = n_im
            prod_re[j, at, :] = q_re
            prod_im[j, at, :] = q_im
            out.append((n_re, n_im, q_re, q_im))
        return tuple(out)

    zero = jnp.zeros((CHUNKS, LANES), jnp.float32)
    one = jnp.ones((CHUNKS, LANES), jnp.float32)
    last = lax.fori_loop(0, length, step, tuple((zero, zero, one, zero) for _ in range(tiles)))
    total = [[], [], [], []]
    read = skip[...] * inputs.astype(jnp.float32)
    for j in range(tiles):
        s_re, s_im, p_re, p_im = last[j]
        a_re, a_im = one[0:1], zero[0:1]
        b_re, b_im = zero[0:1], zero[0:1]
        states_re, states_im = [], []
        for c in range(CHUNKS):
            at = slice(c * length, (c + 1) * length)
            q_re, q_im = prod_re[j, at, :], prod_im[j, at, :]
            states_re.append((run_re[j, at, :] + q_re * b_re - q_im * b_im).astype(jnp.bfloat16))
            states_im.append((run_im[j, at, :] + q_re * b_im + q_im * b_re).astype(jnp.bfloat16))
            whole[0, j, at, :] = (q_re * a_re - q_im * a_im).astype(jnp.bfloat16)
            whole[1, j, at, :] = (q_re * a_im + q_im * a_re).astype(jnp.bfloat16)
            k_re, k_im = p_re[c : c + 1], p_im[c : c + 1]
            b_re, b_im = (
                k_re * b_re - k_im * b_im + s_re[c : c + 1],
                k_re * b_im + k_im * b_re + s_im[c : c + 1],
            )
            a_re, a_im = k_re * a_re - k_im * a_im, k_re * a_im + k_im * a_re
        lanes = slice(j * LANES, (j + 1) * LANES)
        read = read + jnp.dot(jnp.concatenate(states_re, axis=0), read_re[lanes, :], preferred_element_type=jnp.float32)
        read = read - jnp.dot(jnp.concatenate(states_im, axis=0), read_im[lanes, :], preferred_element_type=jnp.float32)
        for kind, row in enumerate((a_re, a_im, b_re, b_im)):
            total[kind].append(row)
    read_local[...] = read
    leaving[0].start()
    leaving[1].start()
    table = jnp.concatenate([row for kind in total for row in kind], axis=0)
    for r in range(devices):
        sent[r] = table
    leaving[2].start()
    for copy in leaving:
        copy.wait()


def state_kernel(devices, index, arrived_out, whole_out, read_out, start, read_re, read_im, out, arrived, whole, read_local, sems):
    me = index[0]
    tiles = whole.shape[1]
    coming = [
        pltpu.make_async_copy(a, b, sems.at[k])
        for k, (a, b) in enumerate(((arrived_out, arrived), (whole_out, whole), (read_out, read_local)))
    ]
    for copy in coming:
        copy.start()
    for copy in coming:
        copy.wait()
    e_re, e_im = start[0:tiles], start[tiles:]
    for z in range(devices - 1):
        a_re, a_im = arrived[z, 0:tiles, :], arrived[z, tiles : 2 * tiles, :]
        b_re, b_im = arrived[z, 2 * tiles : 3 * tiles, :], arrived[z, 3 * tiles :, :]
        n_re = a_re * e_re - a_im * e_im + b_re
        n_im = a_re * e_im + a_im * e_re + b_im
        before = z < me
        e_re, e_im = jnp.where(before, n_re, e_re), jnp.where(before, n_im, e_im)
    read = read_local[...]
    for j in range(tiles):
        p_re, p_im = whole[0, j].astype(jnp.float32), whole[1, j].astype(jnp.float32)
        x_re, x_im = e_re[j : j + 1], e_im[j : j + 1]
        lanes = slice(j * LANES, (j + 1) * LANES)
        late_re = (p_re * x_re - p_im * x_im).astype(jnp.bfloat16)
        late_im = (p_re * x_im + p_im * x_re).astype(jnp.bfloat16)
        read = read + jnp.dot(late_re, read_re[lanes, :], preferred_element_type=jnp.float32)
        read = read - jnp.dot(late_im, read_im[lanes, :], preferred_element_type=jnp.float32)
    out[...] = jax.nn.gelu(read).astype(jnp.bfloat16)


def merge_kernel(taps, index, before, normed, weights, kernel, gain, state_out, other, lhs_mine, rows, gates, merges, padded, rows_in, rows_by_slot, kernel_in, gain_in, sems, small):
    seat = index[2]
    pieces = sems.shape[0] // 2
    high = gates.shape[0] // pieces

    def fetch(to, column, k, sem):
        at = pl.ds(k * high, high)
        return pltpu.make_async_copy(weights.at[at, pl.ds(column * 2 * LANES, 2 * LANES)], to.at[at, :], sems.at[sem])

    for k in range(pieces):
        fetch(gates, 0, k, k).start()
    for k in range(pieces):
        fetch(merges, 1, k, pieces + k).start()
    tiny = [pltpu.make_async_copy(a, b, small.at[k]) for k, (a, b) in enumerate(((kernel, kernel_in), (gain, gain_in)))]
    for copy in tiny:
        copy.start()
    lead = before.shape[0]
    rows[:lead, :] = before[...]
    rows[lead:, :] = normed[...]
    pre = jnp.zeros((rows.shape[0], 2 * LANES), jnp.float32)
    for k in range(pieces):
        fetch(gates, 0, k, k).wait()
        at = slice(k * high, (k + 1) * high)
        pre = pre + jnp.dot(rows[:, at], gates[at, :], preferred_element_type=jnp.float32)
    gated = (pre[:, :LANES] * jax.nn.sigmoid(pre[:, LANES:])).astype(jnp.bfloat16)
    padded[...] = gated.astype(jnp.float32)
    count = state_out.shape[0]
    first = padded.shape[0] - count - (taps - 1)
    for copy in tiny:
        copy.wait()
    by_tap = kernel_in[...].astype(jnp.float32)
    acc = by_tap[0:1] * padded[first : first + count, :]
    for k in range(1, taps):
        acc = acc + by_tap[k : k + 1] * padded[first + k : first + k + count, :]
    center = acc - jnp.mean(acc, axis=1, keepdims=True)
    spread = jnp.mean(center * center, axis=1, keepdims=True)
    normal = center * lax.rsqrt(spread + 1e-05) * gain_in[...]
    rows_in[:, :LANES] = (normal * jax.nn.sigmoid(normal)).astype(jnp.bfloat16)
    rows_in[:, LANES:] = state_out[...]
    seats = 4
    slot = count // (2 * seats)
    core, chip = lax.rem(seat, 2), lax.div(seat, 2)
    for half in range(2):
        wanted = core if half == 0 else 1 - core
        for d in range(seats):
            source = lax.rem(chip + d, seats) * 2 + wanted
            to = (half * seats + d) * slot
            rows_by_slot[to : to + slot, :] = rows_in[pl.ds(pl.multiple_of(source * slot, slot), slot), :]
    lhs_mine[...] = rows_by_slot[: count // 2, :]
    lhs = rows_by_slot[count // 2 :, :]
    for k in range(pieces):
        fetch(merges, 1, k, pieces + k).wait()
    wide = 512
    for f in range(merges.shape[0] // wide):
        at = slice(f * wide, (f + 1) * wide)
        block = lax.dot_general(lhs, merges[at, :], (((1,), (1,)), ((), ())), preferred_element_type=jnp.float32).astype(jnp.bfloat16)
        other[:, at] = block


def own_kernel(lhs, weights, mine, merges, sems):
    pieces = sems.shape[0]
    high = merges.shape[0] // pieces

    def fetch(k):
        at = pl.ds(k * high, high)
        return pltpu.make_async_copy(weights.at[at, pl.ds(2 * LANES, 2 * LANES)], merges.at[at, :], sems.at[k])

    for k in range(pieces):
        fetch(k).start()
    for k in range(pieces):
        fetch(k).wait()
        at = slice(k * high, (k + 1) * high)
        block = lax.dot_general(lhs[...], merges[at, :], (((1,), (1,)), ((), ())), preferred_element_type=jnp.float32)
        mine[:, at] = block.astype(jnp.bfloat16)


def call(kernel, mib, out_shapes, scratch, *args, left=(), kept=False):
    def spec(k, a):
        space = pltpu.SMEM if a.dtype == jnp.int32 else pltpu.HBM if k in left else pltpu.VMEM
        return pl.BlockSpec(memory_space=space)

    return pl.pallas_call(
        kernel,
        out_shape=[jax.ShapeDtypeStruct(*s) for s in out_shapes],
        in_specs=[spec(k, a) for k, a in enumerate(args)],
        out_specs=[pl.BlockSpec(memory_space=pltpu.HBM if kept else pltpu.VMEM) for _ in out_shapes],
        scratch_shapes=[pltpu.VMEM(*s) if isinstance(s, tuple) else s for s in scratch],
        compiler_params=pltpu.CompilerParams(vmem_limit_bytes=mib * 1024 * 1024),
    )(*args)


def body(stream, norm_gain, value_proj, gate_proj, state_proj, conv_kernel, conv_gain, decay_rate, frequency, log_step, step_gain, drive_matrix, read_matrix, skip_gain, start_state, merge_conv, merge_state):
    f32, bf16 = jnp.float32, jnp.bfloat16
    rows, width = stream.shape[1:]
    part = value_proj.shape[0]
    devices, sharers = lax.axis_size("sp"), lax.axis_size("fs")
    index = jnp.stack([lax.axis_index(a) for a in ("sp", "fs", "tp")]).astype(jnp.int32)

    near = from_everyone(jnp.concatenate([value_proj, gate_proj, merge_conv, merge_state], axis=1), "fs")
    near = near.reshape(sharers * part, 4 * LANES)
    near, state_proj = lax.optimization_barrier((near, state_proj))
    weights = lax.all_gather(near, "sp", axis=0, tiled=True)
    column = lax.all_gather(state_proj, "sp", axis=0, tiled=True)
    group_count, state_size = decay_rate.shape
    flat = group_count * state_size
    tiles = flat // LANES
    small = ((tiles, 1, LANES), f32)
    step, rate, turn = call(
        spread_kernel, 4, [((tiles, rows, LANES), f32), small, small], [],
        decay_rate, frequency, log_step[:, None], step_gain[0],
    )
    tokens = stream[0]
    step, tokens, column = lax.optimization_barrier((step, tokens, column))
    pieces = [column] + [shifted(column, "fs", j) for j in range(1, sharers)]
    lead = 32
    normed, tail = call(norm_kernel, 10, [((rows, width), bf16), ((lead, width), bf16)], [], tokens, norm_gain[None])

    modulus = jnp.exp(-step * rate)
    rotation = step * turn
    trans_re = modulus * jnp.cos(rotation)
    trans_im = modulus * jnp.sin(rotation)
    magnitude = rate * rate + turn * turn
    less_re = trans_re - 1.0
    factor_re = (-rate * less_re + turn * trans_im) / magnitude
    factor_im = (-rate * trans_im - turn * less_re) / magnitude
    drive = [block_diagonal(jnp.transpose(drive_matrix[i], (0, 2, 1)).astype(bf16)) for i in range(2)]
    read = [block_diagonal(jnp.transpose(read_matrix[i], (0, 2, 1)).astype(bf16)) for i in range(2)]
    start = start_state[:, 0].reshape(2 * tiles, LANES)

    big = ((tiles, rows, LANES), f32)
    outs = [((rows, LANES), f32), ((2, tiles, rows, LANES), bf16), ((devices, 4 * tiles, LANES), f32)]
    read_local, whole, sent = call(
        functools.partial(scan_kernel, devices, sharers, part),
        20,
        outs,
        [((width, LANES), bf16), big, big, big, big, big, big, *outs, pltpu.SemaphoreType.DMA((3,))],
        index, normed, *read, skip_gain[None], *pieces, trans_re, trans_im, factor_re, factor_im, *drive,
        kept=True,
    )
    sent, tail = lax.optimization_barrier((sent, tail))
    arrived = lax.all_to_all(sent, "sp", split_axis=0, concat_axis=0, tiled=True)
    before = lax.ppermute(tail, "sp", [(i, i + 1) for i in range(devices - 1)])
    (state_out,) = call(
        functools.partial(state_kernel, devices),
        8,
        [((rows, LANES), bf16)],
        [outs[2], outs[1], outs[0], pltpu.SemaphoreType.DMA((3,))],
        index, arrived, whole, read_local, start, *read,
        left=(1, 2, 3),
    )
    copies = 4
    held = pltpu.with_memory_space_constraint(weights, pltpu.HBM)
    other, lhs_mine = call(
        functools.partial(merge_kernel, conv_kernel.shape[0]),
        24,
        [((rows // 2, width), bf16), ((rows // 2, 2 * LANES), bf16)],
        [
            ((rows + lead, width), bf16),
            ((width, 2 * LANES), bf16),
            ((width, 2 * LANES), bf16),
            ((rows + lead, LANES), f32),
            ((rows, 2 * LANES), bf16),
            ((rows, 2 * LANES), bf16),
            (conv_kernel.shape, bf16),
            ((1, LANES), f32),
            pltpu.SemaphoreType.DMA((2 * copies,)),
            pltpu.SemaphoreType.DMA((2,)),
        ],
        index, before, normed, held, conv_kernel, conv_gain[None], state_out,
        left=(3, 4, 5),
    )
    (mine,) = call(
        own_kernel, 12, [((rows // 2, width), bf16)],
        [((width, 2 * LANES), bf16), pltpu.SemaphoreType.DMA((2 * copies,))],
        lhs_mine, held,
        left=(1,),
    )
    got = lax.ppermute(other, "tp", [(i, i ^ 1) for i in range(8)])
    both = (mine.astype(f32) + got.astype(f32)).astype(bf16)
    slot = rows // 8
    mixed = both[:slot].astype(f32)
    for d in (2, 1, 3):
        arriving = shifted(both[d * slot : (d + 1) * slot], "tp", 2 * d)
        mixed = mixed + arriving.astype(f32)
    return mixed.astype(bf16)[None]


def solution(mesh):
    return jax.shard_map(
        body,
        mesh=mesh,
        in_specs=(
            P("fs", "sp", None),
            P(),
            P(("sp", "fs"), "tp"),
            P(("sp", "fs"), "tp"),
            P(("sp", "fs"), "tp"),
            P(None, "tp"),
            P("tp"),
            P("tp", None),
            P("tp", None),
            P("tp"),
            P("fs", "tp", "sp"),
            P(None, "tp", None, None),
            P(None, "tp", None, None),
            P("tp"),
            P(None, "fs", "tp", None),
            P(("sp", "fs"), "tp"),
            P(("sp", "fs"), "tp"),
        ),
        out_specs=P("fs", ("sp", "tp"), None),
        check_vma=False,
    )
```

```python
import functools

import jax
import jax.numpy as jnp
from jax import lax
from jax.experimental import pallas as pl
from jax.experimental.pallas import tpu as pltpu
from jax.sharding import PartitionSpec as P


LANES = 128
CHUNKS = 8


def shifted(array, axis, by):
    devices = lax.axis_size(axis)
    return lax.ppermute(array, axis, [(i, (i + by) % devices) for i in range(devices)])


def from_everyone(array, axis):
    copies = jnp.broadcast_to(array, (lax.axis_size(axis), *array.shape))
    return lax.all_to_all(copies, axis, split_axis=0, concat_axis=0, tiled=True)


def block_diagonal(blocks):
    g, a, b = blocks.shape
    spread = blocks[:, :, None, :] * jnp.eye(g, dtype=blocks.dtype)[:, None, :, None]
    return spread.reshape(g * a, g * b)


def spread_kernel(rates, turns, logs, gains, step, rate, turn):
    groups, size = rates.shape
    per = LANES // size
    by_row = jnp.transpose(jnp.exp(logs[...]) * gains[...])
    lane = lax.broadcasted_iota(jnp.int32, (by_row.shape[0], LANES), 1)
    for j in range(groups // per):
        wide = jnp.broadcast_to(by_row[:, j * per : j * per + 1], lane.shape)
        for k in range(1, per):
            at = j * per + k
            wide = jnp.where(lane < k * size, wide, jnp.broadcast_to(by_row[:, at : at + 1], lane.shape))
        step[j] = wide
        for row, out in ((rates, rate), (turns, turn)):
            out[j] = jnp.concatenate([row[j * per + k : j * per + k + 1, :] for k in range(per)], axis=1)


def norm_kernel(stream, gain, out, tail):
    block = tail.shape[0]

    def step(i, _):
        at = pl.ds(pl.multiple_of(i * block, block), block)
        widened = stream[at, :].astype(jnp.float32)
        inverse = lax.rsqrt(jnp.mean(widened * widened, axis=1, keepdims=True) + 1e-06)
        out[at, :] = (widened * inverse * gain[...]).astype(jnp.bfloat16)
        return 0

    lax.fori_loop(0, stream.shape[0] // block, step, 0)
    tail[...] = out[stream.shape[0] - block :, :]


def scan_kernel(devices, sharers, part, index, normed, read_re, read_im, skip, *refs):
    pieces = refs[:sharers]
    (trans_re, trans_im, factor_re, factor_im, drive_re, drive_im) = refs[sharers : sharers + 6]
    outs = refs[sharers + 6 : sharers + 9]
    weights, push_re, push_im, run_re, run_im, prod_re, prod_im, read_local, whole, sent, sems = refs[sharers + 9 :]
    leaving = [pltpu.make_async_copy(a, b, sems.at[k]) for k, (a, b) in enumerate(zip((read_local, whole, sent), outs))]
    sharer = index[1]
    for j in range(sharers):
        y = lax.rem(sharer - j + sharers, sharers)
        for z in range(devices):
            at = pl.multiple_of(z * sharers * part + y * part, part)
            weights[pl.ds(at, part), :] = pieces[j][z * part : (z + 1) * part, :]
    tiles, count, _ = trans_re.shape
    pre = jnp.dot(normed[...], weights[...], preferred_element_type=jnp.float32)
    inputs = pre.astype(jnp.bfloat16)
    for j in range(tiles):
        lanes = slice(j * LANES, (j + 1) * LANES)
        d_re = jnp.dot(inputs, drive_re[:, lanes], preferred_element_type=jnp.float32)
        d_im = jnp.dot(inputs, drive_im[:, lanes], preferred_element_type=jnp.float32)
        f_re, f_im = factor_re[j], factor_im[j]
        push_re[j] = f_re * d_re - f_im * d_im
        push_im[j] = f_re * d_im + f_im * d_re
    length = count // CHUNKS

    def step(i, carry):
        out = []
        for j in range(tiles):
            s_re, s_im, p_re, p_im = carry[j]
            at = pl.ds(i, CHUNKS, stride=length)
            a_re, a_im = trans_re[j, at, :], trans_im[j, at, :]
            n_re = a_re * s_re - a_im * s_im + push_re[j, at, :]
            n_im = a_re * s_im + a_im * s_re + push_im[j, at, :]
            q_re = a_re * p_re - a_im * p_im
            q_im = a_re * p_im + a_im * p_re
            run_re[j, at, :] = n_re
            run_im[j, at, :] = n_im
            prod_re[j, at, :] = q_re
            prod_im[j, at, :] = q_im
            out.append((n_re, n_im, q_re, q_im))
        return tuple(out)

    zero = jnp.zeros((CHUNKS, LANES), jnp.float32)
    one = jnp.ones((CHUNKS, LANES), jnp.float32)
    last = lax.fori_loop(0, length, step, tuple((zero, zero, one, zero) for _ in range(tiles)))
    total = [[], [], [], []]
    read = skip[...] * inputs.astype(jnp.float32)
    for j in range(tiles):
        s_re, s_im, p_re, p_im = last[j]
        a_re, a_im = one[0:1], zero[0:1]
        b_re, b_im = zero[0:1], zero[0:1]
        states_re, states_im = [], []
        for c in range(CHUNKS):
            at = slice(c * length, (c + 1) * length)
            q_re, q_im = prod_re[j, at, :], prod_im[j, at, :]
            states_re.append((run_re[j, at, :] + q_re * b_re - q_im * b_im).astype(jnp.bfloat16))
            states_im.append((run_im[j, at, :] + q_re * b_im + q_im * b_re).astype(jnp.bfloat16))
            whole[0, j, at, :] = (q_re * a_re - q_im * a_im).astype(jnp.bfloat16)
            whole[1, j, at, :] = (q_re * a_im + q_im * a_re).astype(jnp.bfloat16)
            k_re, k_im = p_re[c : c + 1], p_im[c : c + 1]
            b_re, b_im = (
                k_re * b_re - k_im * b_im + s_re[c : c + 1],
                k_re * b_im + k_im * b_re + s_im[c : c + 1],
            )
            a_re, a_im = k_re * a_re - k_im * a_im, k_re * a_im + k_im * a_re
        lanes = slice(j * LANES, (j + 1) * LANES)
        read = read + jnp.dot(jnp.concatenate(states_re, axis=0), read_re[lanes, :], preferred_element_type=jnp.float32)
        read = read - jnp.dot(jnp.concatenate(states_im, axis=0), read_im[lanes, :], preferred_element_type=jnp.float32)
        for kind, row in enumerate((a_re, a_im, b_re, b_im)):
            total[kind].append(row)
    read_local[...] = read
    leaving[0].start()
    leaving[1].start()
    table = jnp.concatenate([row for kind in total for row in kind], axis=0)
    for r in range(devices):
        sent[r] = table
    leaving[2].start()
    for copy in leaving:
        copy.wait()


def state_kernel(devices, index, arrived_out, whole_out, read_out, start, read_re, read_im, out, arrived, whole, read_local, sems):
    me = index[0]
    tiles = whole.shape[1]
    coming = [
        pltpu.make_async_copy(a, b, sems.at[k])
        for k, (a, b) in enumerate(((arrived_out, arrived), (whole_out, whole), (read_out, read_local)))
    ]
    for copy in coming:
        copy.start()
    for copy in coming:
        copy.wait()
    e_re, e_im = start[0:tiles], start[tiles:]
    for z in range(devices - 1):
        a_re, a_im = arrived[z, 0:tiles, :], arrived[z, tiles : 2 * tiles, :]
        b_re, b_im = arrived[z, 2 * tiles : 3 * tiles, :], arrived[z, 3 * tiles :, :]
        n_re = a_re * e_re - a_im * e_im + b_re
        n_im = a_re * e_im + a_im * e_re + b_im
        before = z < me
        e_re, e_im = jnp.where(before, n_re, e_re), jnp.where(before, n_im, e_im)
    read = read_local[...]
    for j in range(tiles):
        p_re, p_im = whole[0, j].astype(jnp.float32), whole[1, j].astype(jnp.float32)
        x_re, x_im = e_re[j : j + 1], e_im[j : j + 1]
        lanes = slice(j * LANES, (j + 1) * LANES)
        late_re = (p_re * x_re - p_im * x_im).astype(jnp.bfloat16)
        late_im = (p_re * x_im + p_im * x_re).astype(jnp.bfloat16)
        read = read + jnp.dot(late_re, read_re[lanes, :], preferred_element_type=jnp.float32)
        read = read - jnp.dot(late_im, read_im[lanes, :], preferred_element_type=jnp.float32)
    out[...] = jax.nn.gelu(read).astype(jnp.bfloat16)


def merge_kernel(taps, index, before, normed, weights, kernel, gain, state_out, other, lhs_mine, merges, rows, gates, padded, rows_in, rows_by_slot, kernel_in, gain_in, sems, small):
    seat = index[2]
    pieces = sems.shape[0] // 2
    high = gates.shape[0] // pieces

    def fetch(to, column, k, sem):
        at = pl.ds(k * high, high)
        return pltpu.make_async_copy(weights.at[at, pl.ds(column * 2 * LANES, 2 * LANES)], to.at[at, :], sems.at[sem])

    for k in range(pieces):
        fetch(gates, 0, k, k).start()
    for k in range(pieces):
        fetch(merges, 1, k, pieces + k).start()
    tiny = [pltpu.make_async_copy(a, b, small.at[k]) for k, (a, b) in enumerate(((kernel, kernel_in), (gain, gain_in)))]
    for copy in tiny:
        copy.start()
    lead = before.shape[0]
    rows[:lead, :] = before[...]
    rows[lead:, :] = normed[...]
    pre = jnp.zeros((rows.shape[0], 2 * LANES), jnp.float32)
    for k in range(pieces):
        fetch(gates, 0, k, k).wait()
        at = slice(k * high, (k + 1) * high)
        pre = pre + jnp.dot(rows[:, at], gates[at, :], preferred_element_type=jnp.float32)
    gated = (pre[:, :LANES] * jax.nn.sigmoid(pre[:, LANES:])).astype(jnp.bfloat16)
    padded[...] = gated.astype(jnp.float32)
    count = state_out.shape[0]
    first = padded.shape[0] - count - (taps - 1)
    for copy in tiny:
        copy.wait()
    by_tap = kernel_in[...].astype(jnp.float32)
    acc = by_tap[0:1] * padded[first : first + count, :]
    for k in range(1, taps):
        acc = acc + by_tap[k : k + 1] * padded[first + k : first + k + count, :]
    center = acc - jnp.mean(acc, axis=1, keepdims=True)
    spread = jnp.mean(center * center, axis=1, keepdims=True)
    normal = center * lax.rsqrt(spread + 1e-05) * gain_in[...]
    rows_in[:, :LANES] = (normal * jax.nn.sigmoid(normal)).astype(jnp.bfloat16)
    rows_in[:, LANES:] = state_out[...]
    seats = 4
    slot = count // (2 * seats)
    core, chip = lax.rem(seat, 2), lax.div(seat, 2)
    for half in range(2):
        wanted = core if half == 0 else 1 - core
        for d in range(seats):
            source = lax.rem(chip + d, seats) * 2 + wanted
            to = (half * seats + d) * slot
            rows_by_slot[to : to + slot, :] = rows_in[pl.ds(pl.multiple_of(source * slot, slot), slot), :]
    lhs_mine[...] = rows_by_slot[: count // 2, :]
    lhs = rows_by_slot[count // 2 :, :]
    for k in range(pieces):
        fetch(merges, 1, k, pieces + k).wait()
    wide = 512
    for f in range(merges.shape[0] // wide):
        at = slice(f * wide, (f + 1) * wide)
        block = lax.dot_general(lhs, merges[at, :], (((1,), (1,)), ((), ())), preferred_element_type=jnp.float32).astype(jnp.bfloat16)
        other[:, at] = block


def own_kernel(lhs, merges, mine):
    wide = 512
    for f in range(merges.shape[0] // wide):
        at = slice(f * wide, (f + 1) * wide)
        block = lax.dot_general(lhs[...], merges[at, :], (((1,), (1,)), ((), ())), preferred_element_type=jnp.float32)
        mine[:, at] = block.astype(jnp.bfloat16)


def call(kernel, mib, out_shapes, scratch, *args, left=(), kept=False):
    def spec(k, a):
        space = pltpu.SMEM if a.dtype == jnp.int32 else pltpu.HBM if k in left else pltpu.VMEM
        return pl.BlockSpec(memory_space=space)

    return pl.pallas_call(
        kernel,
        out_shape=[jax.ShapeDtypeStruct(*s) for s in out_shapes],
        in_specs=[spec(k, a) for k, a in enumerate(args)],
        out_specs=[pl.BlockSpec(memory_space=pltpu.HBM if kept else pltpu.VMEM) for _ in out_shapes],
        scratch_shapes=[pltpu.VMEM(*s) if isinstance(s, tuple) else s for s in scratch],
        compiler_params=pltpu.CompilerParams(vmem_limit_bytes=mib * 1024 * 1024),
    )(*args)


def body(stream, norm_gain, value_proj, gate_proj, state_proj, conv_kernel, conv_gain, decay_rate, frequency, log_step, step_gain, drive_matrix, read_matrix, skip_gain, start_state, merge_conv, merge_state):
    f32, bf16 = jnp.float32, jnp.bfloat16
    rows, width = stream.shape[1:]
    part = value_proj.shape[0]
    devices, sharers = lax.axis_size("sp"), lax.axis_size("fs")
    index = jnp.stack([lax.axis_index(a) for a in ("sp", "fs", "tp")]).astype(jnp.int32)

    near = from_everyone(jnp.concatenate([value_proj, gate_proj, merge_conv, merge_state], axis=1), "fs")
    near = near.reshape(sharers * part, 4 * LANES)
    near, state_proj = lax.optimization_barrier((near, state_proj))
    weights = lax.all_gather(near, "sp", axis=0, tiled=True)
    column = lax.all_gather(state_proj, "sp", axis=0, tiled=True)
    group_count, state_size = decay_rate.shape
    flat = group_count * state_size
    tiles = flat // LANES
    small = ((tiles, 1, LANES), f32)
    step, rate, turn = call(
        spread_kernel, 4, [((tiles, rows, LANES), f32), small, small], [],
        decay_rate, frequency, log_step[:, None], step_gain[0],
    )
    tokens = stream[0]
    step, tokens, column = lax.optimization_barrier((step, tokens, column))
    pieces = [column] + [shifted(column, "fs", j) for j in range(1, sharers)]
    lead = 32
    normed, tail = call(norm_kernel, 10, [((rows, width), bf16), ((lead, width), bf16)], [], tokens, norm_gain[None])

    modulus = jnp.exp(-step * rate)
    rotation = step * turn
    trans_re = modulus * jnp.cos(rotation)
    trans_im = modulus * jnp.sin(rotation)
    magnitude = rate * rate + turn * turn
    less_re = trans_re - 1.0
    factor_re = (-rate * less_re + turn * trans_im) / magnitude
    factor_im = (-rate * trans_im - turn * less_re) / magnitude
    drive = [block_diagonal(jnp.transpose(drive_matrix[i], (0, 2, 1)).astype(bf16)) for i in range(2)]
    read = [block_diagonal(jnp.transpose(read_matrix[i], (0, 2, 1)).astype(bf16)) for i in range(2)]
    start = start_state[:, 0].reshape(2 * tiles, LANES)

    big = ((tiles, rows, LANES), f32)
    outs = [((rows, LANES), f32), ((2, tiles, rows, LANES), bf16), ((devices, 4 * tiles, LANES), f32)]
    read_local, whole, sent = call(
        functools.partial(scan_kernel, devices, sharers, part),
        20,
        outs,
        [((width, LANES), bf16), big, big, big, big, big, big, *outs, pltpu.SemaphoreType.DMA((3,))],
        index, normed, *read, skip_gain[None], *pieces, trans_re, trans_im, factor_re, factor_im, *drive,
        kept=True,
    )
    sent, tail = lax.optimization_barrier((sent, tail))
    arrived = lax.all_to_all(sent, "sp", split_axis=0, concat_axis=0, tiled=True)
    before = lax.ppermute(tail, "sp", [(i, i + 1) for i in range(devices - 1)])
    (state_out,) = call(
        functools.partial(state_kernel, devices),
        8,
        [((rows, LANES), bf16)],
        [outs[2], outs[1], outs[0], pltpu.SemaphoreType.DMA((3,))],
        index, arrived, whole, read_local, start, *read,
        left=(1, 2, 3),
    )
    copies = 4
    held = pltpu.with_memory_space_constraint(weights, pltpu.HBM)
    other, lhs_mine, merges = call(
        functools.partial(merge_kernel, conv_kernel.shape[0]),
        24,
        [((rows // 2, width), bf16), ((rows // 2, 2 * LANES), bf16), ((width, 2 * LANES), bf16)],
        [
            ((rows + lead, width), bf16),
            ((width, 2 * LANES), bf16),
            ((rows + lead, LANES), f32),
            ((rows, 2 * LANES), bf16),
            ((rows, 2 * LANES), bf16),
            (conv_kernel.shape, bf16),
            ((1, LANES), f32),
            pltpu.SemaphoreType.DMA((2 * copies,)),
            pltpu.SemaphoreType.DMA((2,)),
        ],
        index, before, normed, held, conv_kernel, conv_gain[None], state_out,
        left=(3, 4, 5),
    )
    (mine,) = call(own_kernel, 12, [((rows // 2, width), bf16)], [], lhs_mine, merges)
    got = lax.ppermute(other, "tp", [(i, i ^ 1) for i in range(8)])
    both = (mine.astype(f32) + got.astype(f32)).astype(bf16)
    slot = rows // 8
    mixed = both[:slot].astype(f32)
    for d in (2, 1, 3):
        arriving = shifted(both[d * slot : (d + 1) * slot], "tp", 2 * d)
        if d == 3:
            mixed = lax.optimization_barrier(mixed)
        mixed = mixed + arriving.astype(f32)
    return mixed.astype(bf16)[None]


def solution(mesh):
    return jax.shard_map(
        body,
        mesh=mesh,
        in_specs=(
            P("fs", "sp", None),
            P(),
            P(("sp", "fs"), "tp"),
            P(("sp", "fs"), "tp"),
            P(("sp", "fs"), "tp"),
            P(None, "tp"),
            P("tp"),
            P("tp", None),
            P("tp", None),
            P("tp"),
            P("fs", "tp", "sp"),
            P(None, "tp", None, None),
            P(None, "tp", None, None),
            P("tp"),
            P(None, "fs", "tp", None),
            P(("sp", "fs"), "tp"),
            P(("sp", "fs"), "tp"),
        ),
        out_specs=P("fs", ("sp", "tp"), None),
        check_vma=False,
    )
```
